128 devices in a mesh: sp: 32 (over z, y, core), tp: 4 (over x).
Axes of the slice: x: 4, y: 4, z: 4, core: 2. Of those that a mesh axis runs over, the one named last changes fastest.
Arguments:
- activations: bfloat16 [2, 1024, 1024], P(None, 'sp', 'tp'), may hold values from -6 to 6
- norm_gain: float32 [4, 1024], replicated, may hold values from 0.1 to 1.9
- in_weight: bfloat16 [4, 1024, 512], P(None, 'sp', 'tp'), may hold values from -0.1875 to 0.1875
- out_weight: bfloat16 [4, 512, 1024], P(None, 'tp', 'sp'), may hold values from -0.25 to 0.25
- mixing: bfloat16 [4, 4, 128, 128], P(None, 'tp', 'sp'), may hold values from -0.5 to 0.5
- pool_scale: float32 [4, 512], P(None, 'tp'), may hold values from 0.1 to 1.9
Outputs:
- result: bfloat16 [2, 1024, 1024], P(None, 'sp', 'tp')
The draws below stay inside these ranges and needn't reach their ends.
All inputs are finite; a program needn't handle non-finite values.
Results may differ from the reference program's by a relative error of at most 0.03.
Values may be sent and summed in bfloat16 or wider, within the bound.
A program may use at most 64 MiB of HBM per device.

```python
import jax
import jax.numpy as jnp
from jax import lax

D = 1024
P_SIZE = 512
GROUPS = 4
G = 128
LAYERS = 4
SEQS = 2
SEQ = 1024


def block_scale(own_key, shape, pieces, low, largest):
    level, own = 1.0, jax.random.fold_in(own_key, 6)
    for dim, shards_of in pieces:
        steps = jnp.exp(jax.random.uniform(jax.random.fold_in(own, dim), (shards_of,), jnp.float32, low / len(pieces), largest / len(pieces)))
        level = level * jnp.repeat(steps, shape[dim] // shards_of).reshape([-1 if axis == dim else 1 for axis in range(len(shape))])
    return level


def normal_values(rng, extent, deviation, limit, pieces=(), held_as=jnp.bfloat16):
    drawn = deviation * jax.random.normal(rng, extent, jnp.float32)
    if pieces:
        drawn = drawn * block_scale(rng, extent, pieces, -0.22, 0.18)
    return jnp.clip(drawn, -limit, limit).astype(held_as)


def setup_inputs(seed: int = 0) -> dict:
    arg_keys = jax.random.split(jax.random.key(seed), 7)
    activations = normal_values(arg_keys[0], (SEQS, SEQ, D), 1.0, 6.0, ((1, 32), (2, 4)))
    norm_gain = jnp.clip(1.0 + 0.18 * jax.random.normal(arg_keys[1], (LAYERS, D), jnp.float32), 0.1, 1.9)
    in_weight = normal_values(arg_keys[2], (LAYERS, D, P_SIZE), D ** -0.5, 0.1875, ((1, 32), (2, 4)))
    out_weight = normal_values(arg_keys[3], (LAYERS, P_SIZE, D), P_SIZE ** -0.5, 0.25, ((1, 4), (2, 32)))
    mixing = normal_values(arg_keys[4], (LAYERS, GROUPS, G, G), G ** -0.5, 0.5, ((1, 4), (2, 32)))
    pool_scale = jnp.clip(1.0 + 0.18 * jax.random.normal(arg_keys[5], (LAYERS, P_SIZE), jnp.float32), 0.1, 1.9)
    return dict(activations=activations, norm_gain=norm_gain, in_weight=in_weight, out_weight=out_weight, mixing=mixing, pool_scale=pool_scale)


def pool_layer(activations, norm_gain, in_weight, out_weight, mixing, pool_scale):
    num_seqs, length, model_width = activations.shape
    state_f32 = activations.astype(jnp.float32)
    normed = (state_f32 * lax.rsqrt(lax.optimization_barrier(jnp.mean(state_f32 * state_f32, axis=-1, keepdims=True)) + 1e-06) * norm_gain).astype(jnp.bfloat16)
    flat_rows = normed.reshape(num_seqs * length, model_width)
    pooled_in = jnp.dot(flat_rows, in_weight, preferred_element_type=jnp.float32).astype(jnp.bfloat16)
    pooled_in = pooled_in.reshape(num_seqs, length, -1)
    totals = jnp.pad(jnp.cumsum(pooled_in.astype(jnp.float32), axis=1), ((0, 0), (1, 0), (0, 0)))
    positions = jnp.arange(length, dtype=jnp.int32)
    group_width = mixing.shape[1]
    outputs = []
    for group_slot in range(mixing.shape[0]):
        window = 2 ** (group_slot + 1)
        window_low = jnp.clip(positions - window // 2, 0, length)
        window_high = jnp.clip(positions - window // 2 + window, 0, length)
        columns = slice(group_slot * group_width, (group_slot + 1) * group_width)
        part_sums = totals[:, window_high, columns] - totals[:, window_low, columns]
        window_mean = part_sums / (window_high - window_low).astype(jnp.float32)[None, :, None]
        centred = (window_mean - pooled_in[..., columns].astype(jnp.float32)).astype(jnp.bfloat16)
        mixed_group = jnp.einsum('btc,cd->btd', centred.astype(jnp.float32), mixing[group_slot].astype(jnp.float32))
        outputs.append(mixed_group * pool_scale[columns])
    joined = jnp.concatenate(outputs, axis=-1).astype(jnp.bfloat16).reshape(num_seqs * length, -1)
    next_state = jnp.dot(joined, out_weight, preferred_element_type=jnp.float32).astype(jnp.bfloat16)
    return next_state.reshape(num_seqs, length, model_width)

def reference(activations, norm_gain, in_weight, out_weight, mixing, pool_scale):
    state_now = activations
    for layer_index in range(LAYERS):
        state_now = pool_layer(state_now, norm_gain[layer_index], in_weight[layer_index], out_weight[layer_index], mixing[layer_index], pool_scale[layer_index])
    return state_now
```

```python
import functools

import jax
import jax.numpy as jnp
from jax import lax
from jax.experimental import pallas as pl
from jax.experimental.pallas import tpu as pltpu
from jax.sharding import PartitionSpec as P

F32, BF16 = jnp.float32, jnp.bfloat16
RING = 4
HALO = 8
MIX = 8
ORDERS = ("xyz", "yzx", "zxy", "xyz", "yzx", "zxy", "xyz", "yzx", "zxy")
ROUNDS = ((0, 1, 8, 2), (3, 4, 5), (6, 7))


def kernel(
    act_in, gain_in, w_in, w_out, mix, scale_in, out,
    act, gain, scale, raw, gw, gm, x0, st1, st2, st3, fin, fo,
    s_own, r1, r2, r3, rd, s1, s2, s3, sd, s_act, r_act, s_sc, r_sc, s_h, r_h, s_f, r_f,
):
    layers = gain.shape[0]
    seqs, toks, blk = act.shape
    width = gain.shape[1]
    sp, tp = lax.axis_index("sp"), lax.axis_index("tp")
    sp_size = lax.axis_size("sp")
    c = sp % 2
    me = {"x": tp, "y": (sp // 2) % RING, "z": sp // (2 * RING)}
    seq, half = tp // 2, tp % 2
    seq_len = toks * sp_size
    n0 = x0.shape[1] - 16

    def off(axis, k):
        return lax.rem(me[axis] + (k % RING), RING)

    def device(axis=None, k=0, core=None):
        p = dict(me)
        if axis is not None:
            p[axis] = off(axis, k)
        cc = c if core is None else core
        return {"sp": (p["z"] * RING + p["y"]) * 2 + cc, "tp": p["x"]}

    def near(k):
        return {"sp": lax.rem(sp + k + sp_size, sp_size), "tp": tp}

    partner = device(core=1 - c)

    def remote(src, dst, ss, rs, to):
        return pltpu.make_async_remote_copy(
            src_ref=src, dst_ref=dst, send_sem=ss, recv_sem=rs, device_id=to, device_id_type=pl.DeviceIdType.MESH
        )

    def block(u, sel, r=None, core=None):
        ix = tuple(sel.get(a, slice(None)) for a in "xzy") + (c if core is None else core,)
        if r is not None:
            ix += (r,)
        return gm.at[ix] if u == MIX else gw.at[(u,) + ix]

    def send(ref, ss, rs, to):
        remote(ref, ref, ss, rs, to).start()

    def arrive(ref, rs):
        remote(ref, ref, rs, rs, partner).wait_recv()

    loads = []
    for l in range(layers):
        loads.append(pltpu.make_async_copy(w_in.at[l], gw.at[2 * l, tp, me["z"], me["y"], c], s_own.at[l]))
    loads.append(pltpu.make_async_copy(mix, gm.at[tp, me["z"], me["y"], c], s_own.at[4]))
    loads.append(pltpu.make_async_copy(w_out, raw, s_own.at[5]))
    loads.append(pltpu.make_async_copy(act_in, act, s_own.at[6]))
    loads.append(pltpu.make_async_copy(act_in.at[seq], x0.at[tp, pl.ds(toks, toks)], s_own.at[7]))
    loads.append(pltpu.make_async_copy(scale_in, scale.at[tp], s_own.at[8]))
    loads.append(pltpu.make_async_copy(gain_in, gain, s_own.at[9]))

    barrier = pltpu.get_barrier_semaphore()
    chip_next = {"sp": lax.rem(sp + jnp.where(c == 0, -1, 1) + sp_size, sp_size), "tp": tp}
    everyone = [partner, chip_next] + [device("x", k) for k in (1, 2, 3)]
    everyone += [device(a, k) for a in "yz" for k in (1, 2, 3)]
    for d in everyone:
        pl.semaphore_signal(barrier, inc=1, device_id=d, device_id_type=pl.DeviceIdType.MESH)
    for copy in loads:
        copy.start()
    for copy in loads[:5]:
        copy.wait()
    pl.semaphore_wait(barrier, len(everyone))

    mine = {a: me[a] for a in "xyz"}

    def p1(u):
        a1 = ORDERS[u][0]
        for k in (2, 1, 3):
            send(block(u, mine), s1.at[u], r1.at[u, (-k) % RING], device(a1, k))

    def p1_wait(u):
        a1 = ORDERS[u][0]
        for m in (1, 3, 2):
            arrive(block(u, {**mine, a1: off(a1, m)}), r1.at[u, m])

    def p2(u):
        p1_wait(u)
        a1, a2, a3 = ORDERS[u]
        line = block(u, {a2: me[a2], a3: me[a3]})
        send(line, s2.at[u], r2.at[u, 3], device(a2, 1))
        send(line, s2.at[u], r2.at[u, 1], device(a2, -1))

    def p2_forward(u):
        a1, a2, a3 = ORDERS[u]
        arrive(block(u, {a2: off(a2, 1), a3: me[a3]}), r2.at[u, 1])
        send(block(u, {a2: off(a2, 1), a3: me[a3]}, r=0), s2.at[u], r2.at[u, 2], device(a2, -1))
        arrive(block(u, {a2: off(a2, 3), a3: me[a3]}), r2.at[u, 3])
        send(block(u, {a2: off(a2, 3), a3: me[a3]}, r=1), s2.at[u], r2.at[u, 0], device(a2, 1))

    def p2_opposite(u):
        a1, a2, a3 = ORDERS[u]
        arrive(block(u, {a2: off(a2, 2), a3: me[a3]}, r=0), r2.at[u, 2])
        arrive(block(u, {a2: off(a2, 2), a3: me[a3]}, r=1), r2.at[u, 0])

    def p3(u, j):
        a1, a2, a3 = ORDERS[u]
        ref = block(u, {a2: off(a2, j), a3: me[a3]})
        send(ref, s3.at[u], r3.at[u, j, 3], device(a3, 1))
        send(ref, s3.at[u], r3.at[u, j, 1], device(a3, -1))

    def p3_forward(u, j):
        a1, a2, a3 = ORDERS[u]
        arrive(block(u, {a2: off(a2, j), a3: off(a3, 1)}), r3.at[u, j, 1])
        send(block(u, {a2: off(a2, j), a3: off(a3, 1)}, r=0), s3.at[u], r3.at[u, j, 2], device(a3, -1))
        arrive(block(u, {a2: off(a2, j), a3: off(a3, 3)}), r3.at[u, j, 3])
        send(block(u, {a2: off(a2, j), a3: off(a3, 3)}, r=1), s3.at[u], r3.at[u, j, 0], device(a3, 1))

    def p3_opposite(u):
        a1, a2, a3 = ORDERS[u]
        for j in range(RING):
            arrive(block(u, {a2: off(a2, j), a3: off(a3, 2)}, r=0), r3.at[u, j, 2])
            arrive(block(u, {a2: off(a2, j), a3: off(a3, 2)}, r=1), r3.at[u, j, 0])

    def d2d(u, k):
        a3 = ORDERS[u][2]
        send(block(u, {a3: off(a3, k)}), sd.at[u], rd.at[u], partner)

    def d2d_wait(u):
        arrive(block(u, {}, core=1 - c), rd.at[u])

    def finish_sends(u):
        zero = {"z": 0, "y": 0}
        three = pl.ds(0, 3)
        for ref, sem in (
            (block(u, {**zero, "x": three}), s1), (block(u, {"z": 0, "x": three}), s2),
            (block(u, {"x": three}), s3), (block(u, {}), sd),
        ):
            remote(ref, ref, sem.at[u], sem.at[u], partner).wait_send()

    for u in (0, 8, 2, 4, 6):
        p1(u)
    loads[5].wait()
    for l in range(layers):
        t = raw[l].astype(F32).T.astype(BF16).reshape(2, 16, 128)
        gw[2 * l + 1, tp, me["z"], me["y"], c] = t
    for u in (1, 3, 5, 7):
        p1(u)
    for copy in loads[6:]:
        copy.wait()
    spread = []
    for k in (2, 1, 3):
        t_to = off("x", k)
        m = (-k) % RING
        spread.append(
            remote(act.at[t_to // 2], x0.at[tp, pl.ds(toks, toks)], s_act.at[k], r_act.at[m], device("x", k))
        )
        spread.append(remote(scale.at[tp], scale.at[tp], s_sc.at[k], r_sc.at[m], device("x", k)))
    for copy in spread:
        copy.start()

    has_left, has_right = sp > 0, sp < sp_size - 1
    rows = lambda i: x0.at[:, pl.ds(i * toks, toks)]
    to_right = remote(rows(1), rows(0), s_h.at[0], r_h.at[0], near(1))
    to_left = remote(rows(1), rows(2), s_h.at[1], r_h.at[1], near(-1))

    def blank(i):
        def fill():
            x0[:, i * toks : (i + 1) * toks, :] = jnp.zeros((RING, toks, blk), BF16)

        return fill

    pl.when(jnp.logical_not(has_left))(blank(0))
    pl.when(jnp.logical_not(has_right))(blank(2))

    def halo():
        for m in (1, 3, 2):
            arrive(x0.at[off("x", m), pl.ds(toks, toks)], r_act.at[m])
            arrive(scale.at[off("x", m)], r_sc.at[m])
        pl.when(has_right)(to_right.start)
        pl.when(has_left)(to_left.start)

    def halo_wait():
        pl.when(has_left)(to_right.wait_recv)
        pl.when(has_right)(to_left.wait_recv)

    states = [None, st1, st2, st3]

    def load_rows(l, t):
        n = n0 - 2 * HALO * l
        if l == 0:
            return x0[t, pl.ds(pl.multiple_of(16 * half, 16), n), :]
        return states[l][t]

    def project(l):
        xs = [load_rows(l, t).astype(F32) for t in range(RING)]
        total = sum(jnp.sum(x * x, axis=-1, keepdims=True) for x in xs)
        inv = lax.rsqrt(total * (1.0 / width) + 1e-06)
        normed = jnp.concatenate(
            [(xs[t] * inv * gain[l : l + 1, t * blk : (t + 1) * blk]).astype(BF16) for t in range(RING)], axis=1
        )
        pooled = []
        for p in range(2):
            w = jnp.concatenate([gw[2 * l, 2 * p + i].reshape(width, 128) for i in range(2)], axis=1)
            pooled.append(jnp.dot(normed, w, preferred_element_type=F32).astype(BF16))
        return pooled

    def mixed(l, pooled):
        n_in = n0 - 2 * HALO * l
        n_out = n_in - 2 * HALO
        base = sp * toks + 16 * half - 4 * HALO + HALO * l
        parts = []
        for g in range(RING):
            reach = 2**g
            pos = base + HALO + lax.broadcasted_iota(jnp.int32, (n_out, n_in), 0)
            src = base + lax.broadcasted_iota(jnp.int32, (n_out, n_in), 1)
            low = jnp.maximum(pos - reach, 0)
            high = jnp.minimum(pos + reach, seq_len)
            band = jnp.where((src >= low) & (src < high), 1.0, 0.0).astype(BF16)
            col = base + HALO + lax.broadcasted_iota(jnp.int32, (n_out, 1), 0)
            count = jnp.minimum(col + reach, seq_len) - jnp.maximum(col - reach, 0)
            inv_count = 1.0 / jnp.maximum(count, 1).astype(F32)
            values = pooled[g // 2][:, (g % 2) * 128 : (g % 2 + 1) * 128]
            sums = jnp.dot(band, values, preferred_element_type=F32)
            centred = (sums * inv_count - values.astype(F32)[HALO : HALO + n_out]).astype(BF16)
            m = gm[g, :, :, :, l // 2, l % 2].astype(F32).reshape(128, 128).astype(BF16)
            y = jnp.dot(centred, m, preferred_element_type=F32)
            parts.append((y * scale[g, l : l + 1, :]).astype(BF16))
        return jnp.concatenate(parts, axis=1)

    def out_block(l, joined, q):
        w = jnp.concatenate([gw[2 * l + 1, t, q].reshape(blk, 128) for t in range(RING)], axis=1)
        return lax.dot_general(joined, w, (((1,), (1,)), ((), ())), preferred_element_type=F32).astype(BF16)

    def expand(l, joined):
        for q in range(RING):
            states[l + 1][q] = out_block(l, joined, q)

    r_first, r_second, r_third = ROUNDS
    later = r_second + r_third
    for u in r_first:
        p2(u)
        p3(u, 0)
    halo()
    for u in r_second:
        p2(u)
    for u in r_first:
        p2_forward(u)
        p3(u, 1)
        p3(u, 3)
    for u in r_third:
        p2(u)
    for u in r_first:
        p2_opposite(u)
        p3(u, 2)
        d2d(u, 0)
    for u in r_second:
        p2_forward(u)
    for j in (0, 1, 3):
        for u in r_first:
            p3_forward(u, j)
    for u in r_third:
        p2_forward(u)
    for u in r_first:
        p3_forward(u, 2)
        d2d(u, 1)
        d2d(u, 3)
    for u in r_second:
        p2_opposite(u)
        for j in range(RING):
            p3(u, j)
        d2d(u, 0)
    for u in r_first:
        p3_opposite(u)
        d2d(u, 2)
    for u in r_third:
        p2_opposite(u)
        d2d(u, 0)
    halo_wait()
    d2d_wait(0)
    pooled = project(0)
    d2d_wait(8)
    joined = mixed(0, pooled)
    d2d_wait(1)
    expand(0, joined)
    for u in r_second:
        for j in range(RING):
            p3_forward(u, j)
        d2d(u, 1)
        d2d(u, 3)
    for u in r_third:
        for j in range(RING):
            p3(u, j)
    d2d_wait(2)
    pooled = project(1)
    joined = mixed(1, pooled)
    for u in r_second:
        p3_opposite(u)
        d2d(u, 2)
    d2d_wait(3)
    expand(1, joined)
    for u in r_third:
        for j in range(RING):
            p3_forward(u, j)
        d2d(u, 1)
        d2d(u, 3)
    d2d_wait(4)
    pooled = project(2)
    joined = mixed(2, pooled)
    d2d_wait(5)
    expand(2, joined)
    for u in r_third:
        p3_opposite(u)
        d2d(u, 2)
    d2d_wait(6)
    pooled = project(3)
    joined = mixed(3, pooled)
    d2d_wait(7)
    final = []
    for k in (2, 1, 3, 0):
        q = off("x", k)
        fin[q] = out_block(3, joined, q)
        if k:
            copy = remote(fin.at[q], fo.at[tp], s_f.at[k], r_f.at[(-k) % RING], device("x", k))
            copy.start()
            final.append(copy)
    for u in range(9):
        finish_sends(u)
    for copy in spread:
        copy.wait_send()
    pl.when(has_right)(to_right.wait_send)
    pl.when(has_left)(to_left.wait_send)
    fo[tp] = fin[tp]
    for m in (1, 3, 2):
        arrive(fo.at[off("x", m)], r_f.at[m])
    for s in range(seqs):
        for i in range(2):
            out[s, 16 * i : 16 * (i + 1), :] = fo[2 * s + i]
    for copy in final:
        copy.wait_send()


def body(activations, norm_gain, in_weight, out_weight, mixing, pool_scale):
    layers, in_rows, cols = in_weight.shape
    seqs, toks, blk = activations.shape
    tp_size = lax.axis_size("tp")
    assert (layers, in_rows, cols, seqs, toks, blk, tp_size) == (4, 32, 128, 2, 32, 256, RING)
    in_weight = in_weight.reshape(layers, 2, 16, cols)
    mixing = mixing.reshape(2, 2, 4, cols)
    dma = pltpu.SemaphoreType.DMA
    zs = lax.axis_size("sp") // (2 * RING)
    n0 = toks + 2 * toks
    scratch = [
        pltpu.VMEM(activations.shape, BF16),
        pltpu.VMEM(norm_gain.shape, F32),
        pltpu.VMEM((RING, layers, cols), F32),
        pltpu.VMEM(out_weight.shape, BF16),
        pltpu.VMEM((8, RING, zs, RING, 2, 2, 16, cols), BF16),
        pltpu.VMEM((RING, zs, RING, 2, 2, 2, 4, cols), BF16),
        pltpu.VMEM((RING, n0, blk), BF16),
        pltpu.VMEM((RING, 64, blk), BF16),
        pltpu.VMEM((RING, 48, blk), BF16),
        pltpu.VMEM((RING, 32, blk), BF16),
        pltpu.VMEM((RING, 16, blk), BF16),
        pltpu.VMEM((RING, 16, blk), BF16),
        dma((10,)),
        dma((9, RING)), dma((9, RING)), dma((9, RING, RING)), dma((9,)),
        dma((9,)), dma((9,)), dma((9,)), dma((9,)),
        dma((4,)), dma((4,)), dma((4,)), dma((4,)), dma((2,)), dma((2,)), dma((4,)), dma((4,)),
    ]
    return pl.pallas_call(
        kernel,
        out_shape=jax.ShapeDtypeStruct(activations.shape, BF16),
        in_specs=[pl.BlockSpec(memory_space=pl.ANY)] * 6,
        out_specs=pl.BlockSpec(memory_space=pltpu.VMEM),
        scratch_shapes=scratch,
        compiler_params=pltpu.CompilerParams(collective_id=0, has_side_effects=True),
    )(activations, norm_gain, in_weight, out_weight, mixing, pool_scale)


def solution(mesh):
    return jax.shard_map(
        body,
        mesh=mesh,
        in_specs=(
            P(None, "sp", "tp"),
            P(),
            P(None, "sp", "tp"),
            P(None, "tp", "sp"),
            P(None, "tp", "sp", None),
            P(None, "tp"),
        ),
        out_specs=P(None, "sp", "tp"),
        check_vma=False,
    )
```
